512 devices in a mesh: sp: 64 (over z, y), tp: 8 (over x, core).
Axes of the slice: x: 4, y: 8, z: 8, core: 2. Of those that a mesh axis runs over, the one named last changes fastest.
Arguments:
- latent: bfloat16 [65536, 2048], P('sp'), may hold values from -6 to 6
- context: bfloat16 [1024, 2048], P('sp'), may hold values from -6 to 6
- cond_lat: bfloat16 [2048], P('sp'), may hold values from -6 to 6
- cond_ctx: bfloat16 [2048], P('sp'), may hold values from -6 to 6
- mod_weight: bfloat16 [3, 2048, 2048], P(None, 'sp', 'tp'), may hold values from -0.125 to 0.125
- query_weight: bfloat16 [2048, 1024], P(None, 'tp'), may hold values from -4 to 4
- key_weight: bfloat16 [2048, 512], P(None, 'tp'), may hold values from -4 to 4
- value_weight: bfloat16 [2048, 512], P(None, 'tp'), may hold values from -0.125 to 0.125
- out_weight: bfloat16 [1024, 2048], P(None, 'tp'), may hold values from -1.5 to 1.5
- sink_logit: float32 [16], P('tp'), may hold values from 3 to 6
- context_bias: float32 [16], P('tp'), may hold values from -3.5 to -1.5
Outputs:
- mixed: bfloat16 [65536, 2048], P('sp', 'tp')
The draws below stay inside these ranges and needn't reach their ends.
All inputs are finite; a program needn't handle non-finite values.
Results may differ from the reference program's by a relative error of at most 0.007.
The reference program's roundings to bfloat16 on the way count: a program that leaves them out, or rounds other values in their place, can miss the bound.
Values may be sent and summed in bfloat16 or wider, within the bound.
No kernel may reach another device: no remote copies, remote signals or barrier semaphores. Data moves between devices by JAX's collectives and lax.ppermute only.
A program may use at most 64 MiB of HBM per device.

```python
import math
import jax
import jax.numpy as jnp
from jax import lax

D = 2048
HEADS = 16
KV_HEADS = 8
HEAD_DIM = 64
WINDOW = 128
GRID_W = 64
CTX = 1024
SEQ = 65536
QW = 1024
KVW = 512


def query_key_pair(key):
    query_draw = jax.random.normal(jax.random.fold_in(key, 11), (D, HEADS * HEAD_DIM), jnp.float32) * D ** (-0.5)
    key_draw = jax.random.normal(jax.random.fold_in(key, 12), (D, KV_HEADS * HEAD_DIM), jnp.float32) * D ** (-0.5)
    return (jnp.clip(query_draw, -4.0, 4.0), jnp.clip(key_draw, -4.0, 4.0))


def draw_query_weight(key, part):
    return query_key_pair(key)[0].astype(jnp.bfloat16)


def draw_key_weight(key, part):
    return query_key_pair(key)[1].astype(jnp.bfloat16)


def draw_latent(key, part):
    base_rows = jax.random.normal(jax.random.fold_in(key, 21), (SEQ, D), jnp.float32)
    return jnp.clip(base_rows, -6.0, 6.0).astype(jnp.bfloat16)


def steps_of(own_key, extent, pieces, low, high):
    gain, own = 1.0, jax.random.fold_in(own_key, 6)
    for position, blocks in pieces:
        steps = jnp.exp(jax.random.uniform(jax.random.fold_in(own, position), (blocks,), jnp.float32, low / len(pieces), high / len(pieces)))
        gain = gain * jnp.repeat(steps, extent[position] // blocks).reshape([-1 if axis == position else 1 for axis in range(len(extent))])
    return gain


def bell_draw(stream_key, dims, scale, most, pieces=(), held_as=jnp.bfloat16):
    level = steps_of(stream_key, dims, pieces, -0.22, 0.18) if pieces else 1.0
    drawn = jax.random.normal(stream_key, dims, jnp.float32) * scale * level
    return jnp.minimum(jnp.maximum(drawn, -most), most).astype(held_as)


def setup_inputs(seed: int = 0) -> dict:
    key_of = jax.random.split(jax.random.key(seed), 12)
    return {
        "latent": draw_latent(jax.random.fold_in(key_of[11], 71), 0),
        "context": bell_draw(key_of[1], (CTX, D), 1.0, 6.0, ((0, 64),)),
        "cond_lat": bell_draw(key_of[2], (D,), 1.0, 6.0, ((0, 64),)),
        "cond_ctx": bell_draw(key_of[3], (D,), 1.0, 6.0, ((0, 64),)),
        "mod_weight": bell_draw(key_of[4], (3, D, D), D ** -0.5, 0.125, ((1, 64), (2, 8))),
        "query_weight": draw_query_weight(jax.random.fold_in(key_of[11], 71), 0),
        "key_weight": draw_key_weight(jax.random.fold_in(key_of[11], 71), 0),
        "value_weight": bell_draw(key_of[7], (D, KVW), D ** -0.5, 0.125, ((1, 8),)),
        "out_weight": bell_draw(key_of[8], (QW, D), (QW // 64) ** -0.5, 1.5, ((1, 8),)),
        "sink_logit": jnp.clip(3.0 + 3.0 * jax.random.uniform(key_of[9], (HEADS,), jnp.float32) ** steps_of(key_of[9], (HEADS,), ((0, 8),), -0.2, 0.2), 3.0, 6.0),
        "context_bias": jnp.clip(-3.5 + 2.0 * jax.random.uniform(key_of[10], (HEADS,), jnp.float32) ** steps_of(key_of[10], (HEADS,), ((0, 8),), -0.2, 0.2), -3.5, -1.5),
    }


norm_eps = 1e-05
rope_base = 10000.0

def rotary_tables(positions):
    grid_row = (positions // GRID_W).astype(jnp.float32)
    grid_col = (positions % GRID_W).astype(jnp.float32)
    freq_count = HEAD_DIM // 4
    inverse = rope_base ** (-jnp.arange(freq_count, dtype=jnp.float32) / freq_count)
    angles = jnp.concatenate([grid_row[:, None] * inverse, grid_col[:, None] * inverse], axis=-1)
    return (jnp.cos(angles), jnp.sin(angles))

def rotate(vectors, cos_table, sin_table):
    half_dim = vectors.shape[-1] // 2
    first_half = vectors[..., :half_dim]
    second_half = vectors[..., half_dim:]
    return jnp.concatenate([first_half * cos_table - second_half * sin_table, first_half * sin_table + second_half * cos_table], axis=-1)

def modulate(row_block, shift_scale):
    values_f = row_block.astype(jnp.float32)
    center = lax.optimization_barrier(jnp.mean(values_f, -1, keepdims=True))
    spread = lax.optimization_barrier(jnp.mean(jnp.square(values_f - center), -1, keepdims=True))
    normed = (values_f - center) * lax.rsqrt(spread + norm_eps)
    return (normed * (1.0 + shift_scale[1]) + shift_scale[0]).astype(jnp.bfloat16)

def softmax_parts(window_scores, context_scores, sinks):
    top_logit = jnp.maximum(jnp.maximum(lax.optimization_barrier(jnp.max(window_scores, -1)), lax.optimization_barrier(jnp.max(context_scores, -1))), sinks[:, :, None])
    window_exp = jnp.exp(window_scores - top_logit[..., None])
    context_exp = jnp.exp(context_scores - top_logit[..., None])
    denominator = lax.optimization_barrier(jnp.sum(window_exp, -1)) + lax.optimization_barrier(jnp.sum(context_exp, -1)) + jnp.exp(sinks[:, :, None] - top_logit)
    return ((window_exp / denominator[..., None]).astype(jnp.bfloat16), (context_exp / denominator[..., None]).astype(jnp.bfloat16))

def reference(latent, context, cond_lat, cond_ctx, mod_weight, query_weight, key_weight, value_weight, out_weight, sink_logit, context_bias):
    group_size = HEADS // KV_HEADS
    scale = HEAD_DIM ** (-0.5)
    activated = jax.nn.silu(jnp.stack([cond_lat, cond_ctx]).astype(jnp.float32)).astype(jnp.bfloat16)
    modulation = jnp.einsum('cd,rde->cre', activated.astype(jnp.float32), mod_weight.astype(jnp.float32))
    normed = modulate(latent, modulation[0])
    context_normed = modulate(context, modulation[1])
    positions = jnp.arange(SEQ, dtype=jnp.int32)
    cos_table, sin_table = rotary_tables(positions)
    query_full = jnp.dot(normed, query_weight, preferred_element_type=jnp.float32).reshape(SEQ, HEADS, HEAD_DIM)
    key_full = jnp.dot(normed, key_weight, preferred_element_type=jnp.float32).reshape(SEQ, KV_HEADS, HEAD_DIM)
    queries = rotate(query_full, cos_table[:, None, :], sin_table[:, None, :]).astype(jnp.bfloat16)
    keys = rotate(key_full, cos_table[:, None, :], sin_table[:, None, :]).astype(jnp.bfloat16)
    values = jnp.dot(normed, value_weight, preferred_element_type=jnp.float32).astype(jnp.bfloat16)
    values = values.reshape(SEQ, KV_HEADS, HEAD_DIM)
    context_keys = jnp.dot(context_normed, key_weight, preferred_element_type=jnp.float32).astype(jnp.bfloat16)
    context_keys = context_keys.reshape(CTX, KV_HEADS, HEAD_DIM).astype(jnp.float32)
    context_values = jnp.dot(context_normed, value_weight, preferred_element_type=jnp.float32).astype(jnp.bfloat16)
    context_values = context_values.reshape(CTX, KV_HEADS, HEAD_DIM).astype(jnp.float32)
    padded_keys = jnp.pad(keys, ((WINDOW, WINDOW), (0, 0), (0, 0)))
    padded_values = jnp.pad(values, ((WINDOW, WINDOW), (0, 0), (0, 0)))
    grouped = queries.reshape(SEQ, KV_HEADS, group_size, HEAD_DIM)
    sinks = sink_logit.astype(jnp.float32).reshape(KV_HEADS, group_size)
    biases = context_bias.astype(jnp.float32).reshape(KV_HEADS, group_size)
    block_rows = math.gcd(SEQ, 512)
    block_count = SEQ // block_rows
    span = block_rows + 2 * WINDOW

    def one_block(block_index):
        first = (block_index * block_rows).astype(jnp.int32)
        block_queries = lax.dynamic_slice_in_dim(grouped, first, block_rows, 0).astype(jnp.float32)
        block_keys = lax.dynamic_slice_in_dim(padded_keys, first, span, 0).astype(jnp.float32)
        block_values = lax.dynamic_slice_in_dim(padded_values, first, span, 0).astype(jnp.float32)
        query_pos = first + jnp.arange(block_rows, dtype=jnp.int32)
        key_pos = first - WINDOW + jnp.arange(span, dtype=jnp.int32)
        valid = (jnp.abs(query_pos[:, None] - key_pos[None, :]) <= WINDOW) & (key_pos >= 0)[None, :] & (key_pos < SEQ)[None, :]
        window_scores = jnp.einsum('qgrd,kgd->grqk', block_queries, block_keys) * scale
        window_scores = jnp.where(valid, window_scores, -jnp.inf)
        context_scores = jnp.einsum('qgrd,cgd->grqc', block_queries, context_keys) * scale + biases[:, :, None, None]
        window_weights, context_weights = softmax_parts(window_scores, context_scores, sinks)
        attended = jnp.einsum('grqk,kgd->qgrd', window_weights.astype(jnp.float32), block_values) + jnp.einsum('grqc,cgd->qgrd', context_weights.astype(jnp.float32), context_values)
        return attended.reshape(block_rows, QW).astype(jnp.bfloat16)
    attended = lax.map(one_block, jnp.arange(block_count, dtype=jnp.int32)).reshape(SEQ, QW)
    projected = jnp.dot(attended, out_weight, preferred_element_type=jnp.float32)
    return (latent.astype(jnp.float32) + modulation[0, 2] * projected).astype(jnp.bfloat16)
```

```python
import jax
import jax.numpy as jnp
from jax import lax
from jax.sharding import PartitionSpec as P

HEAD_DIM = 64
WINDOW = 128
GRID_W = 64
CORES = 2


norm_eps = 1e-05
rope_base = 10000.0


def copy_for_each(shard, axis):
    copies = jnp.broadcast_to(shard, (lax.axis_size(axis), *shard.shape))
    return lax.all_to_all(copies, axis, split_axis=0, concat_axis=0, tiled=True)


def of_everyone(shard, axis):
    everything = copy_for_each(shard, axis)
    return jnp.sum(everything, axis=0)


def joined_along(parts, dim):
    dims = list(parts.shape[1:])
    dims[dim] *= parts.shape[0]
    return jnp.moveaxis(parts, 0, dim).reshape(dims)


def gathered_copies(shard, axis, dim):
    return joined_along(copy_for_each(shard, axis), dim)


def neighbour_rows(rows, width, axis):
    count = lax.axis_size(axis)
    forward = [(i, i + 1) for i in range(count - 1)]
    backward = [(target, source) for source, target in forward]
    low = lax.ppermute(rows[rows.shape[0] - width :], axis, forward)
    high = lax.ppermute(rows[:width], axis, backward)
    return jnp.concatenate([low, high], axis=0)


def same_core_copies(shard, axis):
    count = lax.axis_size(axis)
    groups = [list(range(core, count, CORES)) for core in range(CORES)]
    copies = jnp.broadcast_to(shard, (count // CORES, *shard.shape))
    return lax.all_to_all(
        copies, axis, split_axis=0, concat_axis=0, tiled=True, axis_index_groups=groups
    )


def swapped_cores(block, axis):
    count = lax.axis_size(axis)
    return lax.ppermute(block, axis, [(i, i ^ 1) for i in range(count)])


def rotary_tables(positions):
    grid_row = (positions // GRID_W).astype(jnp.float32)
    grid_col = (positions % GRID_W).astype(jnp.float32)
    freq_count = HEAD_DIM // 4
    inverse = rope_base ** (-jnp.arange(freq_count, dtype=jnp.float32) / freq_count)
    angles = jnp.concatenate([grid_row[:, None] * inverse, grid_col[:, None] * inverse], axis=-1)
    return (jnp.cos(angles), jnp.sin(angles))


def rotate(vectors, cos_table, sin_table):
    half_dim = vectors.shape[-1] // 2
    first_half = vectors[..., :half_dim]
    second_half = vectors[..., half_dim:]
    return jnp.concatenate(
        [
            first_half * cos_table - second_half * sin_table,
            first_half * sin_table + second_half * cos_table,
        ],
        axis=-1,
    )


def modulate(row_block, shift_scale):
    values_f = row_block.astype(jnp.float32)
    center = jnp.mean(values_f, -1, keepdims=True)
    spread = jnp.mean(jnp.square(values_f - center), -1, keepdims=True)
    normed = (values_f - center) * lax.rsqrt(spread + norm_eps)
    return (normed * (1.0 + shift_scale[1]) + shift_scale[0]).astype(jnp.bfloat16)


def softmax_parts(window_scores, context_scores, sinks):
    top_logit = jnp.maximum(
        jnp.maximum(jnp.max(window_scores, -1), jnp.max(context_scores, -1)), sinks[:, :, None]
    )
    window_exp = jnp.exp(window_scores - top_logit[..., None])
    context_exp = jnp.exp(context_scores - top_logit[..., None])
    denominator = (
        jnp.sum(window_exp, -1) + jnp.sum(context_exp, -1) + jnp.exp(sinks[:, :, None] - top_logit)
    )
    return (
        (window_exp / denominator[..., None]).astype(jnp.bfloat16),
        (context_exp / denominator[..., None]).astype(jnp.bfloat16),
    )


def attend_block(
    block_queries, block_keys, block_values, context_keys, context_values, valid, sinks, biases
):
    scale = HEAD_DIM ** (-0.5)
    window_scores = (
        jnp.einsum("qgrd,kgd->grqk", block_queries, block_keys, preferred_element_type=jnp.float32)
        * scale
    )
    window_scores = jnp.where(valid, window_scores, -jnp.inf)
    context_scores = (
        jnp.einsum(
            "qgrd,cgd->grqc", block_queries, context_keys, preferred_element_type=jnp.float32
        )
        * scale
    )
    context_scores = context_scores + biases[:, :, None, None]
    window_weights, context_weights = softmax_parts(window_scores, context_scores, sinks)
    attended = jnp.einsum(
        "grqk,kgd->qgrd", window_weights, block_values, preferred_element_type=jnp.float32
    ) + jnp.einsum(
        "grqc,cgd->qgrd", context_weights, context_values, preferred_element_type=jnp.float32
    )
    return attended.astype(jnp.bfloat16)


def on_device(
    latent,
    context,
    cond_lat,
    cond_ctx,
    mod_weight,
    query_weight,
    key_weight,
    value_weight,
    out_weight,
    sink_logit,
    context_bias,
):
    tokens_here = latent.shape[0]
    column_count = out_weight.shape[1]
    column_index = lax.axis_index("tp")
    query_cols = query_weight.shape[1]
    key_cols = key_weight.shape[1]
    heads_kv = key_cols // HEAD_DIM
    group_size = query_cols // key_cols
    activated = jax.nn.silu(jnp.stack([cond_lat, cond_ctx]).astype(jnp.float32)).astype(
        jnp.bfloat16
    )
    partial_mod = jnp.einsum(
        "cd,rde->cre", activated, mod_weight, preferred_element_type=jnp.float32
    )
    halo_rows = neighbour_rows(latent, WINDOW, "sp")
    summed_mod = of_everyone(partial_mod, "sp")
    modulation = gathered_copies(summed_mod, "tp", 2)
    kv_weight = jnp.concatenate([key_weight, value_weight], axis=1)
    context_normed = modulate(context, modulation[1])
    context_kv = gathered_copies(
        jnp.dot(context_normed, kv_weight, preferred_element_type=jnp.float32).astype(jnp.bfloat16),
        "sp",
        0,
    )
    context_count = context_kv.shape[0]
    context_keys = context_kv[:, :key_cols].reshape(context_count, heads_kv, HEAD_DIM)
    context_values = context_kv[:, key_cols:].reshape(context_count, heads_kv, HEAD_DIM)
    normed = modulate(latent, modulation[0])
    merged_weight = jnp.concatenate([query_weight, key_weight, value_weight], axis=1)
    projections = jnp.dot(normed, merged_weight, preferred_element_type=jnp.float32)
    halo_kv = jnp.dot(
        modulate(halo_rows, modulation[0]), kv_weight, preferred_element_type=jnp.float32
    )
    offset = lax.axis_index("sp") * tokens_here
    seq_total = tokens_here * lax.axis_size("sp")
    positions = offset - WINDOW + jnp.arange(tokens_here + 2 * WINDOW, dtype=jnp.int32)
    cos_table, sin_table = rotary_tables(positions)
    own = slice(WINDOW, WINDOW + tokens_here)
    queries = rotate(
        projections[:, :query_cols].reshape(tokens_here, heads_kv * group_size, HEAD_DIM),
        cos_table[own, None, :],
        sin_table[own, None, :],
    ).astype(jnp.bfloat16)
    queries = queries.reshape(tokens_here, heads_kv, group_size, HEAD_DIM)
    kv_rows = jnp.concatenate(
        [halo_kv[:WINDOW], projections[:, query_cols:], halo_kv[WINDOW:]], axis=0
    )
    keys = rotate(
        kv_rows[:, :key_cols].reshape(-1, heads_kv, HEAD_DIM),
        cos_table[:, None, :],
        sin_table[:, None, :],
    ).astype(jnp.bfloat16)
    values = kv_rows[:, key_cols:].astype(jnp.bfloat16)
    extended = jnp.concatenate([keys.reshape(-1, key_cols), values], axis=1)
    sinks = sink_logit.reshape(heads_kv, group_size)
    biases = context_bias.reshape(heads_kv, group_size)
    block_rows = min(512, tokens_here)
    span = block_rows + 2 * WINDOW
    outputs = []
    for block_index in range(tokens_here // block_rows):
        first_row = block_index * block_rows
        block_kv = extended[first_row : first_row + span]
        block_keys = block_kv[:, :key_cols].reshape(span, heads_kv, HEAD_DIM)
        block_values = block_kv[:, key_cols:].reshape(span, heads_kv, HEAD_DIM)
        query_pos = offset + first_row + jnp.arange(block_rows, dtype=jnp.int32)
        key_pos = offset + first_row - WINDOW + jnp.arange(span, dtype=jnp.int32)
        valid = (
            (jnp.abs(query_pos[:, None] - key_pos[None, :]) <= WINDOW)
            & (key_pos >= 0)[None, :]
            & (key_pos < seq_total)[None, :]
        )
        block_out = attend_block(
            queries[first_row : first_row + block_rows],
            block_keys,
            block_values,
            context_keys,
            context_values,
            valid,
            sinks,
            biases,
        )
        outputs.append(block_out.reshape(block_rows, query_cols))
    attended = jnp.concatenate(outputs, axis=0)
    core = column_index % CORES
    weight_by_core = out_weight.reshape(-1, CORES, query_cols, column_count)
    own_core_weight = lax.dynamic_index_in_dim(weight_by_core, core, 1, keepdims=False)
    other_core_weight = lax.dynamic_index_in_dim(weight_by_core, 1 - core, 1, keepdims=False)
    from_chips = same_core_copies(attended, "tp")
    from_other = swapped_cores(from_chips, "tp")
    projected = jnp.einsum(
        "xrk,xkn->rn", from_chips, own_core_weight, preferred_element_type=jnp.float32
    ) + jnp.einsum(
        "xrk,xkn->rn", from_other, other_core_weight, preferred_element_type=jnp.float32
    )
    own_columns = lax.dynamic_slice_in_dim(latent, column_index * column_count, column_count, 1)
    gate_columns = lax.dynamic_slice_in_dim(
        modulation[0, 2], column_index * column_count, column_count, 0
    )
    return (own_columns.astype(jnp.float32) + gate_columns * projected).astype(jnp.bfloat16)


def solution(mesh):
    return jax.shard_map(
        on_device,
        mesh=mesh,
        in_specs=(
            P("sp", None),
            P("sp", None),
            P("sp"),
            P("sp"),
            P(None, "sp", "tp"),
            P(None, "tp"),
            P(None, "tp"),
            P(None, "tp"),
            P(None, "tp"),
            P("tp"),
            P("tp"),
        ),
        out_specs=P("sp", "tp"),
        check_vma=False,
    )
```

```python
import functools

import jax
import jax.numpy as jnp
from jax import lax
from jax.experimental import pallas as pl
from jax.experimental.pallas import tpu as pltpu
from jax.sharding import PartitionSpec as P

HEAD_DIM = 64
WINDOW = 128
GRID_W = 64
CORES = 2
STEP_ROWS = 2 * WINDOW
NORM_ROWS = 16


norm_eps = 1e-05
rope_base = 10000.0


def copy_for_each(shard, axis):
    copies = jnp.broadcast_to(shard, (lax.axis_size(axis), *shard.shape))
    return lax.all_to_all(copies, axis, split_axis=0, concat_axis=0, tiled=True)


def of_everyone(shard, axis):
    everything = copy_for_each(shard, axis)
    return jnp.sum(everything, axis=0)


def joined_along(parts, dim):
    dims = list(parts.shape[1:])
    dims[dim] *= parts.shape[0]
    return jnp.moveaxis(parts, 0, dim).reshape(dims)


def gathered_copies(shard, axis, dim):
    return joined_along(copy_for_each(shard, axis), dim)


def neighbour_rows(rows, width, axis):
    count = lax.axis_size(axis)
    forward = [(i, i + 1) for i in range(count - 1)]
    backward = [(target, source) for source, target in forward]
    low = lax.ppermute(rows[rows.shape[0] - width :], axis, forward)
    high = lax.ppermute(rows[:width], axis, backward)
    return jnp.concatenate([low, high], axis=0)


def from_same_cores(copies, axis):
    count = lax.axis_size(axis)
    groups = [list(range(core, count, CORES)) for core in range(CORES)]
    return lax.all_to_all(
        copies, axis, split_axis=0, concat_axis=0, tiled=True, axis_index_groups=groups
    )


def swapped_cores(block, axis):
    count = lax.axis_size(axis)
    return lax.ppermute(block, axis, [(i, i ^ 1) for i in range(count)])


def rotary_tables(positions):
    grid_row = (positions // GRID_W).astype(jnp.float32)
    grid_col = (positions % GRID_W).astype(jnp.float32)
    freq_count = HEAD_DIM // 4
    inverse = rope_base ** (-jnp.arange(freq_count, dtype=jnp.float32) / freq_count)
    angles = jnp.concatenate([grid_row[:, None] * inverse, grid_col[:, None] * inverse], axis=-1)
    return (jnp.cos(angles), jnp.sin(angles))


def modulate(row_block, shift_scale):
    values_f = row_block.astype(jnp.float32)
    center = jnp.mean(values_f, -1, keepdims=True)
    spread = jnp.mean(jnp.square(values_f - center), -1, keepdims=True)
    normed = (values_f - center) * lax.rsqrt(spread + norm_eps)
    return (normed * (1.0 + shift_scale[1]) + shift_scale[0]).astype(jnp.bfloat16)


def rotated_columns(vectors, cos_table, sin_table):
    half_dim = vectors.shape[0] // 2
    first_half = vectors[:half_dim]
    second_half = vectors[half_dim:]
    return jnp.concatenate(
        [
            first_half * cos_table - second_half * sin_table,
            first_half * sin_table + second_half * cos_table,
        ],
        axis=0,
    )


def window_kernel(
    start_ref,
    latent_ref,
    halo_ref,
    weight_ref,
    shift_ref,
    gain_ref,
    cos_ref,
    sin_ref,
    queries_ref,
    partial_ref,
    stats_ref,
    normed_ref,
    keys_ref,
    values_ref,
    *,
    tokens,
    seq_total,
):
    step = pl.program_id(0)
    own_steps = tokens // STEP_ROWS
    width = weight_ref.shape[1]
    group = weight_ref.shape[0] // HEAD_DIM - 2
    lanes = group * WINDOW

    def project(rows_ref):
        def normalise(index, carry):
            first = pl.multiple_of(index * NORM_ROWS, NORM_ROWS)
            rows = rows_ref[pl.ds(first, NORM_ROWS), :].astype(jnp.float32)
            center = jnp.sum(rows, axis=1, keepdims=True) * (1.0 / width)
            rows = rows - center
            spread = jnp.sum(rows * rows, axis=1, keepdims=True) * (1.0 / width)
            rows = rows * lax.rsqrt(spread + norm_eps)
            normed_ref[pl.ds(first, NORM_ROWS), :] = (
                rows * gain_ref[...] + shift_ref[...]
            ).astype(jnp.bfloat16)
            return carry

        lax.fori_loop(0, STEP_ROWS // NORM_ROWS, normalise, 0, unroll=2)
        return lax.dot_general(
            weight_ref[...],
            normed_ref[...],
            (((1,), (1,)), ((), ())),
            preferred_element_type=jnp.float32,
        )

    def keys_of(columns, cos_table, sin_table):
        rotated = rotated_columns(columns, cos_table, sin_table)
        return jnp.transpose(rotated).astype(jnp.bfloat16)

    key_row = group * HEAD_DIM
    value_row = key_row + HEAD_DIM

    @pl.when(step < own_steps)
    def _():
        columns = project(latent_ref)
        first = pl.multiple_of(WINDOW + step * STEP_ROWS, WINDOW)
        cos_table = cos_ref[:, pl.ds(first, STEP_ROWS)]
        sin_table = sin_ref[:, pl.ds(first, STEP_ROWS)]
        keys_ref[pl.ds(first, STEP_ROWS), :] = keys_of(
            columns[key_row:value_row], cos_table, sin_table
        )
        values = columns[value_row:].astype(jnp.bfloat16)
        values_ref[:, pl.ds(first, STEP_ROWS)] = values
        for head in range(group):
            rotated = rotated_columns(
                columns[head * HEAD_DIM : (head + 1) * HEAD_DIM], cos_table, sin_table
            )
            rotated = rotated.astype(jnp.bfloat16) * jnp.bfloat16(HEAD_DIM**-0.5)
            for part in range(STEP_ROWS // WINDOW):
                queries_ref[
                    step * (STEP_ROWS // WINDOW) + part, :, head * WINDOW : (head + 1) * WINDOW
                ] = rotated[:, part * WINDOW : (part + 1) * WINDOW]

    @pl.when(step == own_steps)
    def _():
        columns = project(halo_ref)
        last = WINDOW + tokens
        for first, part in ((0, 0), (last, WINDOW)):
            here = columns[:, part : part + WINDOW]
            keys_ref[first : first + WINDOW, :] = keys_of(
                here[key_row:value_row],
                cos_ref[:, first : first + WINDOW],
                sin_ref[:, first : first + WINDOW],
            )
            values_ref[:, first : first + WINDOW] = here[value_row:].astype(jnp.bfloat16)
        span = 3 * WINDOW
        key_index = lax.broadcasted_iota(jnp.int32, (span, lanes), 0)
        query_index = lax.broadcasted_iota(jnp.int32, (span, lanes), 1) % WINDOW
        band = (key_index >= query_index) & (key_index <= query_index + 2 * WINDOW)

        def attend(block, carry):
            row = pl.multiple_of(block * WINDOW, WINDOW)
            key_start = start_ref[0] + row - WINDOW
            scores = jnp.dot(
                keys_ref[pl.ds(row, span), :],
                queries_ref[block],
                preferred_element_type=jnp.float32,
            )
            valid = band & (key_index >= -key_start) & (key_index < seq_total - key_start)
            scores = jnp.where(valid, scores, -jnp.inf)
            top = jnp.max(scores, axis=0, keepdims=True)
            weights = jnp.exp(scores - top)
            stats_ref[block, 0:1, :] = top
            stats_ref[block, 1:2, :] = jnp.sum(weights, axis=0, keepdims=True)
            partial_ref[block] = jnp.dot(
                values_ref[:, pl.ds(row, span)],
                weights.astype(jnp.bfloat16),
                preferred_element_type=jnp.float32,
            )
            return carry

        lax.fori_loop(0, tokens // WINDOW, attend, 0)


def context_kernel(
    queries_ref, partial_ref, stats_ref, context_ref, sink_ref, bias_ref, out_ref, values_ref
):
    group = queries_ref.shape[2] // WINDOW

    @pl.when(pl.program_id(0) == 0)
    def _():
        both = jnp.transpose(context_ref[...].astype(jnp.float32))
        values_ref[...] = both[HEAD_DIM:].astype(jnp.bfloat16)

    scores = jnp.dot(
        context_ref[:, :HEAD_DIM], queries_ref[0], preferred_element_type=jnp.float32
    )
    bias = bias_ref[...]
    sink = sink_ref[...]
    window_top = stats_ref[0, 0:1, :]
    top = jnp.maximum(
        jnp.maximum(jnp.max(scores, axis=0, keepdims=True) + bias, window_top), sink
    )
    weights = jnp.exp(scores - (top - bias))
    window_share = jnp.exp(window_top - top)
    total = (
        jnp.sum(weights, axis=0, keepdims=True)
        + stats_ref[0, 1:2, :] * window_share
        + jnp.exp(sink - top)
    )
    mixed = (
        jnp.dot(values_ref[...], weights.astype(jnp.bfloat16), preferred_element_type=jnp.float32)
        + partial_ref[0] * window_share
    )
    mixed = mixed / total
    heads = [mixed[:, head * WINDOW : (head + 1) * WINDOW] for head in range(group)]
    rows = jnp.transpose(jnp.concatenate(heads, axis=0)).astype(jnp.bfloat16)
    for copy in range(out_ref.shape[0]):
        out_ref[copy] = rows


def on_device(
    latent,
    context,
    cond_lat,
    cond_ctx,
    mod_weight,
    query_weight,
    key_weight,
    value_weight,
    out_weight,
    sink_logit,
    context_bias,
):
    tokens_here = latent.shape[0]
    column_count = out_weight.shape[1]
    column_index = lax.axis_index("tp")
    query_cols = query_weight.shape[1]
    key_cols = key_weight.shape[1]
    group_size = query_cols // key_cols
    activated = jax.nn.silu(jnp.stack([cond_lat, cond_ctx]).astype(jnp.float32)).astype(
        jnp.bfloat16
    )
    partial_mod = jnp.einsum(
        "cd,rde->cre", activated, mod_weight, preferred_element_type=jnp.float32
    )
    halo_rows = neighbour_rows(latent, WINDOW, "sp")
    summed_mod = of_everyone(partial_mod, "sp")
    modulation = gathered_copies(summed_mod, "tp", 2)
    kv_weight = jnp.concatenate([key_weight, value_weight], axis=1)
    context_normed = modulate(context, modulation[1])
    context_kv = gathered_copies(
        jnp.dot(context_normed, kv_weight, preferred_element_type=jnp.float32).astype(jnp.bfloat16),
        "sp",
        0,
    )
    offset = lax.axis_index("sp") * tokens_here
    seq_total = tokens_here * lax.axis_size("sp")
    positions = offset - WINDOW + jnp.arange(tokens_here + 2 * WINDOW, dtype=jnp.int32)
    cos_table, sin_table = rotary_tables(positions)
    weight_rows = jnp.concatenate([query_weight.T, key_weight.T, value_weight.T], axis=0)
    own_steps = tokens_here // STEP_ROWS
    blocks = tokens_here // WINDOW
    lanes = group_size * WINDOW
    features = latent.shape[1]
    whole = lambda *shape: pl.BlockSpec(shape, lambda i: (0,) * len(shape))
    queries, partial, stats = pl.pallas_call(
        functools.partial(window_kernel, tokens=tokens_here, seq_total=seq_total),
        grid=(own_steps + 1,),
        in_specs=[
            pl.BlockSpec(memory_space=pltpu.SMEM),
            pl.BlockSpec((STEP_ROWS, features), lambda i: (jnp.minimum(i, own_steps - 1), 0)),
            whole(STEP_ROWS, features),
            whole(*weight_rows.shape),
            whole(1, features),
            whole(1, features),
            whole(HEAD_DIM // 2, tokens_here + 2 * WINDOW),
            whole(HEAD_DIM // 2, tokens_here + 2 * WINDOW),
        ],
        out_specs=[
            whole(blocks, HEAD_DIM, lanes),
            whole(blocks, HEAD_DIM, lanes),
            whole(blocks, 8, lanes),
        ],
        out_shape=[
            jax.ShapeDtypeStruct((blocks, HEAD_DIM, lanes), jnp.bfloat16),
            jax.ShapeDtypeStruct((blocks, HEAD_DIM, lanes), jnp.float32),
            jax.ShapeDtypeStruct((blocks, 8, lanes), jnp.float32),
        ],
        scratch_shapes=[
            pltpu.VMEM((STEP_ROWS, features), jnp.bfloat16),
            pltpu.VMEM((tokens_here + 2 * WINDOW, HEAD_DIM), jnp.bfloat16),
            pltpu.VMEM((HEAD_DIM, tokens_here + 2 * WINDOW), jnp.bfloat16),
        ],
        name="window_part",
    )(
        offset.reshape(1),
        latent,
        halo_rows,
        weight_rows,
        modulation[0, 0][None],
        1.0 + modulation[0, 1][None],
        cos_table.T,
        sin_table.T,
    )
    chips = lax.axis_size("tp") // CORES
    attended = pl.pallas_call(
        context_kernel,
        grid=(blocks,),
        in_specs=[
            pl.BlockSpec((1, HEAD_DIM, lanes), lambda i: (i, 0, 0)),
            pl.BlockSpec((1, HEAD_DIM, lanes), lambda i: (i, 0, 0)),
            pl.BlockSpec((1, 8, lanes), lambda i: (i, 0, 0)),
            whole(*context_kv.shape),
            whole(1, lanes),
            whole(1, lanes),
        ],
        out_specs=pl.BlockSpec((chips, WINDOW, query_cols), lambda i: (0, i, 0)),
        out_shape=jax.ShapeDtypeStruct((chips, tokens_here, query_cols), jnp.bfloat16),
        scratch_shapes=[pltpu.VMEM((HEAD_DIM, context_kv.shape[0]), jnp.bfloat16)],
        name="context_part",
    )(
        queries,
        partial,
        stats,
        context_kv,
        jnp.repeat(sink_logit, WINDOW)[None],
        jnp.repeat(context_bias, WINDOW)[None],
    )
    core = column_index % CORES
    weight_by_core = out_weight.reshape(-1, CORES, query_cols, column_count)
    own_core_weight = lax.dynamic_index_in_dim(weight_by_core, core, 1, keepdims=False)
    other_core_weight = lax.dynamic_index_in_dim(weight_by_core, 1 - core, 1, keepdims=False)
    from_chips = from_same_cores(attended, "tp")
    from_other = swapped_cores(from_chips, "tp")
    projected = jnp.einsum(
        "xrk,xkn->rn", from_chips, own_core_weight, preferred_element_type=jnp.float32
    ) + jnp.einsum(
        "xrk,xkn->rn", from_other, other_core_weight, preferred_element_type=jnp.float32
    )
    own_columns = lax.dynamic_slice_in_dim(latent, column_index * column_count, column_count, 1)
    gate_columns = lax.dynamic_slice_in_dim(
        modulation[0, 2], column_index * column_count, column_count, 0
    )
    return (own_columns.astype(jnp.float32) + gate_columns * projected).astype(jnp.bfloat16)


def solution(mesh):
    return jax.shard_map(
        on_device,
        mesh=mesh,
        in_specs=(
            P("sp", None),
            P("sp", None),
            P("sp"),
            P("sp"),
            P(None, "sp", "tp"),
            P(None, "tp"),
            P(None, "tp"),
            P(None, "tp"),
            P(None, "tp"),
            P("tp"),
            P("tp"),
        ),
        out_specs=P("sp", "tp"),
        check_vma=False,
    )
```
